32 devices in a mesh: fs: 8 (over z, y), tp: 4 (over x, core).
Axes of the slice: x: 2, y: 2, z: 4, core: 2. Of those that a mesh axis runs over, the one named last changes fastest.
Arguments:
- normed_input: bfloat16 [36864, 2048], P('fs'), may hold values from -8 to 8
- query_latent_cotangent: bfloat16 [36864, 768], P('fs', 'tp'), may hold values from -0.03125 to 0.03125
- key_value_latent_cotangent: bfloat16 [36864, 512], P('fs', 'tp'), may hold values from -0.03125 to 0.03125
- row_factor: bfloat16 [2048, 256], P('fs'), may hold values from -0.1875 to 0.1875
- query_down_weight: float32 [2048, 768], P('fs', 'tp'), may hold values from -6 to 6
- key_value_down_weight: float32 [2048, 512], P('fs', 'tp'), may hold values from -6 to 6
- query_first_moment: float32 [256, 768], P('fs', 'tp'), may hold values from -6 to 6
- key_value_first_moment: float32 [256, 512], P('fs', 'tp'), may hold values from -6 to 6
- query_second: float32 [256, 768], P('fs', 'tp'), may hold values from 0.5 to 2000
- latent_second: float32 [256, 512], P('fs', 'tp'), may hold values from 0.5 to 2000
Outputs:
- query_new: float32 [2048, 768], P('fs', 'tp')
- latent_new: float32 [2048, 512], P('fs', 'tp')
- query_step: float32 [2048, 768], P('fs', 'tp')
- latent_step: float32 [2048, 512], P('fs', 'tp')
- query_copy: bfloat16 [2048, 768], P(None, 'tp')
- latent_copy: bfloat16 [2048, 512], P(None, 'tp')
- query_first_new: float32 [256, 768], P('fs', 'tp')
- latent_first_new: float32 [256, 512], P('fs', 'tp')
- query_second_new: float32 [256, 768], P('fs', 'tp')
- latent_second_new: float32 [256, 512], P('fs', 'tp')
The draws below stay inside these ranges and needn't reach their ends.
All inputs are finite; a program needn't handle non-finite values.
Results may differ from the reference program's by a relative error of at most 0.006.
Values may be sent and summed in bfloat16 or wider, within the bound.
A program may use at most 64 MiB of HBM per device.

```python
import jax
import jax.numpy as jnp
from jax import lax

MODEL_WIDTH = 2048
QUERY_LATENT = 768
KEY_VALUE_LATENT = 512
PROJECTION_RANK = 256
TOKEN_TOTAL = 36864


def second_moment_estimate(key, rows, cols):
    key_two = jax.random.fold_in(key, 1)
    row_index = jnp.arange(rows, dtype=jnp.float32) / max(rows - 1, 1)
    col_index = jnp.arange(cols, dtype=jnp.float32) / max(cols - 1, 1)
    col_scale = 10.0 ** col_index
    row_scale = 100.0 ** row_index
    jitter = jnp.exp(jax.random.uniform(key_two, (rows, cols), jnp.float32, -0.69, 0.69))
    return row_scale[:, None] * col_scale[None, :] * jitter


def draw_query_second(key, part):
    return second_moment_estimate(jax.random.fold_in(key, 11), PROJECTION_RANK, QUERY_LATENT)


def draw_latent_second(key, part):
    return second_moment_estimate(jax.random.fold_in(key, 12), PROJECTION_RANK, KEY_VALUE_LATENT)


def spiked(values, key, source, target, blocks, factor):
    owner, partner = [(jnp.arange(values.shape[position]) // (values.shape[position] // blocks)).reshape([-1 if axis == position else 1 for axis in range(values.ndim)]) for position in (source, target)]
    chosen = jax.random.permutation(key, blocks)[partner]
    strong = (owner == chosen) | (owner == (partner + blocks // 2) % blocks)
    return jnp.where(strong, factor * values, values)


def block_levels(key, shape, shards, low, top_value):
    factor_of, own = 1.0, jax.random.fold_in(key, 6)
    for dim, parts in shards:
        draws = jnp.exp(jax.random.uniform(jax.random.fold_in(own, dim), (parts,), jnp.float32, low / len(shards), top_value / len(shards)))
        factor_of = factor_of * jnp.repeat(draws, shape[dim] // parts).reshape([-1 if axis == dim else 1 for axis in range(len(shape))])
    return factor_of


def centred(key, shape, scale, bound, cuts=(), kind=jnp.bfloat16):
    result = jax.random.normal(key, shape, jnp.float32) * scale
    if len(cuts) > 0:
        result = block_levels(key, shape, cuts, -0.22, 0.18) * result
    return jnp.clip(result, min=-bound, max=bound).astype(kind)


def gaussian_with(own_key, dims, scale, limit, pieces, heavy, kind=jnp.bfloat16):
    result = scale * jax.random.normal(own_key, dims, jnp.float32)
    if pieces:
        result = result * block_levels(own_key, dims, pieces, -0.22, 0.18)
    return jnp.clip(spiked(result, jax.random.fold_in(own_key, 3), *heavy), -limit, limit).astype(kind)


def setup_inputs(seed: int = 0) -> dict:
    keys = jax.random.split(jax.random.key(seed), 11)
    return {
        "normed_input": gaussian_with(keys[0], (TOKEN_TOTAL, MODEL_WIDTH), 1.0, 8.0, ((0, 8),), (0, 1, 8, 2.0)),
        "query_latent_cotangent": centred(keys[1], (TOKEN_TOTAL, QUERY_LATENT), (TOKEN_TOTAL ** -0.5), 0.03125, ((0, 8), (1, 4))),
        "key_value_latent_cotangent": centred(keys[2], (TOKEN_TOTAL, KEY_VALUE_LATENT), (TOKEN_TOTAL ** -0.5), 0.03125, ((0, 8), (1, 4))),
        "row_factor": gaussian_with(keys[3], (MODEL_WIDTH, PROJECTION_RANK), MODEL_WIDTH ** -0.5, 0.1875, ((0, 8),), (0, 1, 8, 2.0)),
        "query_down_weight": centred(keys[4], (MODEL_WIDTH, QUERY_LATENT), 1.0, 6.0, ((0, 8), (1, 4)), jnp.float32),
        "key_value_down_weight": centred(keys[5], (MODEL_WIDTH, KEY_VALUE_LATENT), 1.0, 6.0, ((0, 8), (1, 4)), jnp.float32),
        "query_first_moment": centred(keys[6], (PROJECTION_RANK, QUERY_LATENT), 1.0, 6.0, ((0, 8), (1, 4)), jnp.float32),
        "key_value_first_moment": centred(keys[7], (PROJECTION_RANK, KEY_VALUE_LATENT), 1.0, 6.0, ((0, 8), (1, 4)), jnp.float32),
        "query_second": draw_query_second(jax.random.fold_in(keys[10], 71), 0),
        "latent_second": draw_latent_second(jax.random.fold_in(keys[10], 71), 0),
    }


def token_sum(left, right):
    return lax.dot_general(left, right, (((0,), (0,)), ((), ())), preferred_element_type=jnp.float32)

def update_one(gradient, factor32, weight, first, second):
    projected = jnp.dot(factor32.T, gradient, precision=lax.Precision.HIGHEST)
    first_new = 0.8 * first + 0.2 * projected
    second_new = 0.9 * second + 0.1 * projected * projected
    direction = first_new / (jnp.sqrt(second_new) + 1e-08)
    count = direction.shape[0] * direction.shape[1]
    scale = 0.5 * jnp.sqrt(jnp.float32(count)) / jnp.sqrt(jnp.sum(direction * direction) + 1e-06)
    step = jnp.dot(factor32, scale * direction, precision=lax.Precision.HIGHEST)
    weight_new = weight - step
    return (weight_new, step, weight_new.astype(jnp.bfloat16), first_new, second_new)

def reference(normed_input, query_latent_cotangent, key_value_latent_cotangent, row_factor, query_down_weight, key_value_down_weight, query_first_moment, key_value_first_moment, query_second, latent_second):
    factor32 = row_factor.astype(jnp.float32)
    grad_q = token_sum(normed_input, query_latent_cotangent)
    grad_kv = token_sum(normed_input, key_value_latent_cotangent)
    qn, qs, qc, qf, qv = update_one(grad_q, factor32, query_down_weight, query_first_moment, query_second)
    kn, ks, kc, kf, kv = update_one(grad_kv, factor32, key_value_down_weight, key_value_first_moment, latent_second)
    return (qn, kn, qs, ks, qc, kc, qf, kf, qv, kv)
```

```python
import functools

import jax
import jax.numpy as jnp
from jax import lax
from jax.experimental import pallas as pl
from jax.experimental.pallas import tpu as pltpu
from jax.sharding import PartitionSpec as P

MESH = pl.DeviceIdType.MESH
F32 = jnp.float32
BF16 = jnp.bfloat16


def kernel(
    n,
    tp,
    chunks,
    x_hbm,
    cq_hbm,
    ck_hbm,
    p_hbm,
    wq_ref,
    wk_ref,
    mq_ref,
    mk_ref,
    vq_ref,
    vk_ref,
    qnew_ref,
    knew_ref,
    qstep_ref,
    kstep_ref,
    qcopy_ref,
    kcopy_ref,
    qfirst_ref,
    kfirst_ref,
    qsecond_ref,
    ksecond_ref,
    xs,
    cqs,
    cks,
    acc,
    pall,
    wall,
    rs_mine,
    rs_send,
    rs_recv,
    dall,
    sums,
    x_sem,
    c_sem,
    p_local,
    p_send,
    p_recv,
    s_send,
    s_recv,
    w_send,
    w_recv,
    rs_ssem,
    rs_rsem,
    d_send,
    d_recv,
    q_send,
    q_recv,
):
    f = lax.axis_index("fs")
    t = lax.axis_index("tp")
    depth = n // 2
    col, side = f // 2, f % 2
    half = t % 2
    sibling = t + 1 - 2 * half
    across = f + 1 - 2 * side
    me = f * tp + t
    qw = wq_ref.shape[1]
    kw = wk_ref.shape[1]
    rr = mq_ref.shape[0]
    rows = wq_ref.shape[0]

    barrier = pltpu.get_barrier_semaphore()
    for i in range(n):
        for j in range(tp):
            if i or j:
                pl.semaphore_signal(
                    barrier,
                    inc=1,
                    device_id=(lax.rem(f + i, n), lax.rem(t + j, tp)),
                    device_id_type=MESH,
                )

    p_copy = pltpu.make_async_copy(p_hbm, pall.at[f], p_local)
    p_copy.start()
    cq_copy = pltpu.make_async_copy(cq_hbm, cqs, c_sem.at[0])
    ck_copy = pltpu.make_async_copy(ck_hbm, cks, c_sem.at[1])
    cq_copy.start()
    ck_copy.start()

    def x_copy(i):
        return pltpu.make_async_copy(x_hbm.at[i], xs.at[i], x_sem.at[i])

    for i in range(chunks):
        x_copy(i).start()

    wall[f] = jnp.concatenate([wq_ref[...], wk_ref[...]], axis=1).astype(BF16)
    acc[...] = jnp.zeros_like(acc)

    def remote(src, dst, ssem, rsem, to):
        return pltpu.make_async_remote_copy(
            src_ref=src, dst_ref=dst, send_sem=ssem, recv_sem=rsem, device_id=to, device_id_type=MESH
        )

    def p_fs(block, slot, to):
        ref = pall.at[block, half]
        return remote(ref, ref, p_send.at[slot], p_recv.at[block], (to, t))

    def p_tp(block, slot):
        ref = pall.at[block, half]
        return remote(ref, ref, s_send.at[slot], s_recv.at[block], (f, sibling))

    def w_fs(block, slot, to):
        ref = wall.at[block]
        return remote(ref, ref, w_send.at[slot], w_recv.at[block], (to, t))

    def column(k):
        return lax.rem(col + k, depth) * 2 + side

    def other(k):
        return lax.rem(col + k, depth) * 2 + 1 - side

    sends = []

    def go(copy):
        copy.start()
        sends.append(copy)

    def multiply(i, carry):
        x_copy(i).wait()
        left = jnp.concatenate([cqs[i].T, cks[i].T], axis=0)
        acc[...] += jnp.dot(left, xs[i], preferred_element_type=F32)
        return carry

    p_copy.wait()
    pl.semaphore_wait(barrier, n * tp - 1)
    for k in range(1, depth):
        go(p_fs(f, k - 1, column(k)))
    go(p_fs(f, depth - 1, across))
    go(w_fs(f, 0, across))
    if depth > 1:
        go(w_fs(f, 1, column(1)))

    cq_copy.wait()
    ck_copy.wait()
    first = (2 * chunks) // 3
    lax.fori_loop(0, first, multiply, 0)
    slot = depth
    for k in range(depth - 1, 0, -1):
        block = column(k)
        p_fs(block, 0, across).wait_recv()
        go(p_fs(block, slot, across))
        slot += 1
        go(p_tp(block, k))
    lax.fori_loop(first, chunks, multiply, 0)
    for k in range(depth):
        block = other(k)
        p_fs(block, 0, across).wait_recv()
        go(p_tp(block, depth + k))
    for k in range(depth):
        if k > 0:
            remote(pall.at[column(k), 1 - half], pall.at[column(k), 1 - half], s_send.at[0], s_recv.at[column(k)], (f, sibling)).wait_recv()
        remote(pall.at[other(k), 1 - half], pall.at[other(k), 1 - half], s_send.at[0], s_recv.at[other(k)], (f, sibling)).wait_recv()

    whole_p = pall[...].reshape(n * rows, pall.shape[-1])
    projected = jnp.dot(acc[...].astype(BF16), whole_p, preferred_element_type=F32).T
    for k in range(n):
        piece = projected[k * rr : (k + 1) * rr]
        rs_mine[k] = piece
        rs_send[k] = piece.astype(BF16)
    for k in range(1, n):
        to = lax.rem(f + k, n)
        go(remote(rs_send.at[to], rs_recv.at[f], rs_ssem.at[k], rs_rsem.at[f], (to, t)))
    total = rs_mine[f]
    for k in range(1, n):
        src = lax.rem(f + n - k, n)
        remote(rs_recv.at[src], rs_recv.at[src], rs_ssem.at[0], rs_rsem.at[src], (f, sibling)).wait_recv()
        total = total + rs_recv[src].astype(F32)

    def moment_update(part, first_ref, second_ref, first_out, second_out):
        first_new = 0.8 * first_ref[...] + 0.2 * part
        second_new = 0.9 * second_ref[...] + 0.1 * part * part
        first_out[...] = first_new
        second_out[...] = second_new
        return first_new / (jnp.sqrt(second_new) + 1e-08)

    dir_q = moment_update(total[:, :qw], mq_ref, vq_ref, qfirst_ref, qsecond_ref)
    dir_k = moment_update(total[:, qw:], mk_ref, vk_ref, kfirst_ref, ksecond_ref)
    dall[f] = jnp.concatenate([dir_q, dir_k], axis=1).astype(BF16)
    lane = lax.broadcasted_iota(jnp.int32, (1, 128), 1)
    sums[me] = jnp.where(lane < 64, jnp.sum(dir_q * dir_q), jnp.sum(dir_k * dir_k))
    for k in range(1, n):
        to = lax.rem(f + k, n)
        go(remote(dall.at[f], dall.at[f], d_send.at[k], d_recv.at[f], (to, t)))
    for i in range(n):
        for j in range(tp):
            if i or j:
                to = (lax.rem(f + i, n), lax.rem(t + j, tp))
                go(remote(sums.at[me], sums.at[me], q_send.at[i * tp + j], q_recv.at[me], to))

    for k in range(2, depth):
        go(w_fs(f, k, column(k)))
    slot = depth
    for k in range(depth - 1, 0, -1):
        block = column(k)
        w_fs(block, 0, across).wait_recv()
        go(w_fs(block, slot, across))
        slot += 1

    for k in range(1, n):
        src = lax.rem(f + n - k, n)
        remote(dall.at[src], dall.at[src], d_send.at[0], d_recv.at[src], (f, sibling)).wait_recv()
    for i in range(n):
        for j in range(tp):
            if i or j:
                src = lax.rem(f + i, n) * tp + lax.rem(t + j, tp)
                remote(sums.at[src], sums.at[src], q_send.at[0], q_recv.at[src], (f, sibling)).wait_recv()
    row = jnp.sum(sums[...], axis=0)
    q_sq = row[:, 0:1]
    k_sq = row[:, 64:65]
    q_count = jnp.float32(n * rr * qw * tp)
    k_count = jnp.float32(n * rr * kw * tp)
    q_scale = 0.5 * jnp.sqrt(q_count) / jnp.sqrt(q_sq + 1e-06)
    k_scale = 0.5 * jnp.sqrt(k_count) / jnp.sqrt(k_sq + 1e-06)
    lanes = lax.broadcasted_iota(jnp.int32, (1, qw + kw), 1)
    scale = jnp.where(lanes < qw, q_scale, k_scale)
    dirs = jnp.concatenate([dall[k].astype(F32) for k in range(n)], axis=0).astype(BF16)
    mine = pall[f].reshape(rows, pall.shape[-1])
    step = jnp.dot(mine, dirs, preferred_element_type=F32) * scale
    qstep_ref[...] = step[:, :qw]
    kstep_ref[...] = step[:, qw:]
    qnew_ref[...] = wq_ref[...] - step[:, :qw]
    knew_ref[...] = wk_ref[...] - step[:, qw:]

    for k in range(depth):
        block = other(k)
        w_fs(block, 0, across).wait_recv()

    def finish(i, carry):
        step = jnp.dot(pall[i].reshape(rows, pall.shape[-1]), dirs, preferred_element_type=F32) * scale
        new = wall[i].astype(F32) - step
        at = pl.ds(pl.multiple_of(i * rows, rows), rows)
        qcopy_ref[at, :] = new[:, :qw].astype(BF16)
        kcopy_ref[at, :] = new[:, qw:].astype(BF16)
        return carry

    lax.fori_loop(0, n, finish, 0)
    for copy in sends:
        copy.wait_send()


def solution(mesh):
    n, tp = mesh.shape["fs"], mesh.shape["tp"]

    def body(x, cq, ck, factor, wq, wk, mq, mk, vq, vk):
        tokens, width = x.shape
        rows, rank = factor.shape
        qw, kw = wq.shape[1], wk.shape[1]
        lat = qw + kw
        rr = mq.shape[0]
        chunk = 512
        while tokens % chunk:
            chunk //= 2
        chunks = tokens // chunk
        vmem = pl.BlockSpec(memory_space=pltpu.VMEM)
        anys = pl.BlockSpec(memory_space=pl.ANY)
        dma = pltpu.SemaphoreType.DMA
        sds = jax.ShapeDtypeStruct
        return pl.pallas_call(
            functools.partial(kernel, n, tp, chunks),
            out_shape=(
                sds((rows, qw), F32),
                sds((rows, kw), F32),
                sds((rows, qw), F32),
                sds((rows, kw), F32),
                sds((n * rows, qw), BF16),
                sds((n * rows, kw), BF16),
                sds((rr, qw), F32),
                sds((rr, kw), F32),
                sds((rr, qw), F32),
                sds((rr, kw), F32),
            ),
            in_specs=[anys] * 4 + [vmem] * 6,
            out_specs=(vmem,) * 10,
            scratch_shapes=[
                pltpu.VMEM((chunks, chunk, width), BF16),
                pltpu.VMEM((chunks, chunk, qw), BF16),
                pltpu.VMEM((chunks, chunk, kw), BF16),
                pltpu.VMEM((lat, width), F32),
                pltpu.VMEM((n, 2, rows // 2, rank), BF16),
                pltpu.VMEM((n, rows, lat), BF16),
                pltpu.VMEM((n, rr, lat), F32),
                pltpu.VMEM((n, rr, lat), BF16),
                pltpu.VMEM((n, rr, lat), BF16),
                pltpu.VMEM((n, rr, lat), BF16),
                pltpu.VMEM((n * tp, 1, 128), F32),
                dma((chunks,)),
                dma((2,)),
                dma(()),
                dma((n,)),
                dma((n,)),
                dma((n,)),
                dma((n,)),
                dma((n,)),
                dma((n,)),
                dma((n,)),
                dma((n,)),
                dma((n,)),
                dma((n,)),
                dma((n * tp,)),
                dma((n * tp,)),
            ],
            compiler_params=pltpu.CompilerParams(
                collective_id=0, has_side_effects=True, vmem_limit_bytes=58 * 1024 * 1024
            ),
        )(
            x.reshape(chunks, chunk, width),
            cq.reshape(chunks, chunk, qw),
            ck.reshape(chunks, chunk, kw),
            factor.reshape(2, rows // 2, rank),
            wq,
            wk,
            mq,
            mk,
            vq,
            vk,
        )

    return jax.shard_map(
        body,
        mesh=mesh,
        in_specs=(P("fs", None), P("fs", "tp"), P("fs", "tp"), P("fs", None)) + (P("fs", "tp"),) * 6,
        out_specs=(P("fs", "tp"),) * 4 + (P(None, "tp"),) * 2 + (P("fs", "tp"),) * 4,
        check_vma=False,
    )
```

```python
import functools

import jax
import jax.numpy as jnp
from jax import lax
from jax.experimental import pallas as pl
from jax.experimental.pallas import tpu as pltpu
from jax.sharding import PartitionSpec as P

MESH = pl.DeviceIdType.MESH
F32 = jnp.float32
BF16 = jnp.bfloat16


def directions(total, qw, mq_ref, mk_ref, vq_ref, vk_ref):
    def update(part, first, second):
        first_new = 0.8 * first + 0.2 * part
        second_new = 0.9 * second + 0.1 * part * part
        return first_new, second_new, first_new / (jnp.sqrt(second_new) + 1e-08)

    return (
        update(total[:, :qw], mq_ref[...], vq_ref[...]),
        update(total[:, qw:], mk_ref[...], vk_ref[...]),
    )


def exchange(
    n,
    tp,
    chunks,
    x_hbm,
    cq_hbm,
    ck_hbm,
    p_hbm,
    wq_ref,
    wk_ref,
    mq_ref,
    mk_ref,
    vq_ref,
    vk_ref,
    pall,
    wqall,
    wkall,
    dall,
    sums,
    total_ref,
    xs,
    cqs,
    cks,
    acc,
    rs_mine,
    rs_send,
    rs_recv,
    x_sem,
    c_sem,
    p_local,
    p_send,
    p_recv,
    s_send,
    s_recv,
    w_send,
    w_recv,
    v_send,
    v_recv,
    rs_ssem,
    rs_rsem,
    d_send,
    d_recv,
    q_send,
    q_recv,
):
    f = lax.axis_index("fs")
    t = lax.axis_index("tp")
    depth = n // 2
    col, side = f // 2, f % 2
    half = t % 2
    sibling = t + 1 - 2 * half
    across = f + 1 - 2 * side
    me = f * tp + t
    qw = mq_ref.shape[1]
    rr = mq_ref.shape[0]
    rows = wk_ref.shape[0]
    chunk = xs.shape[1]

    barrier = pltpu.get_barrier_semaphore()
    for i in range(n):
        for j in range(tp):
            if i or j:
                pl.semaphore_signal(
                    barrier,
                    inc=1,
                    device_id=(lax.rem(f + i, n), lax.rem(t + j, tp)),
                    device_id_type=MESH,
                )

    p_copy = pltpu.make_async_copy(p_hbm, pall.at[f], p_local)
    p_copy.start()
    cq_copy = pltpu.make_async_copy(cq_hbm, cqs, c_sem.at[0])
    ck_copy = pltpu.make_async_copy(ck_hbm, cks, c_sem.at[1])
    cq_copy.start()
    ck_copy.start()

    def x_copy(i):
        return pltpu.make_async_copy(x_hbm.at[i], xs.at[i], x_sem.at[i])

    for i in range(chunks):
        x_copy(i).start()

    wqall[f] = wq_ref[...].astype(BF16)
    wkall[f] = wk_ref[...].astype(BF16)
    acc[...] = jnp.zeros_like(acc)

    def remote(src, dst, ssem, rsem, to):
        return pltpu.make_async_remote_copy(
            src_ref=src, dst_ref=dst, send_sem=ssem, recv_sem=rsem, device_id=to, device_id_type=MESH
        )

    def p_fs(block, slot, to):
        ref = pall.at[block, half]
        return remote(ref, ref, p_send.at[slot], p_recv.at[block], (to, t))

    def p_tp(block, slot):
        ref = pall.at[block, half]
        return remote(ref, ref, s_send.at[slot], s_recv.at[block], (f, sibling))

    def w_fs(block, slot, to):
        q, v = wqall.at[block], wkall.at[block]
        return (
            remote(q, q, w_send.at[slot], w_recv.at[block], (to, t)),
            remote(v, v, v_send.at[slot], v_recv.at[block], (to, t)),
        )

    def w_go(block, slot, to):
        for copy in w_fs(block, slot, to):
            go(copy)

    def w_wait(block):
        for copy in w_fs(block, 0, across):
            copy.wait_recv()

    def column(k):
        return lax.rem(col + k, depth) * 2 + side

    def other(k):
        return lax.rem(col + k, depth) * 2 + 1 - side

    sends = []

    def go(copy):
        copy.start()
        sends.append(copy)

    def multiply(i, carry):
        x_copy(i).wait()
        at = pl.ds(pl.multiple_of(i * chunk, chunk), chunk)
        left = jnp.concatenate([cqs[:, at], cks[i].T], axis=0)
        acc[...] += jnp.dot(left, xs[i], preferred_element_type=F32)
        return carry

    p_copy.wait()
    pl.semaphore_wait(barrier, n * tp - 1)
    for k in range(1, depth):
        go(p_fs(f, k - 1, column(k)))
    go(p_fs(f, depth - 1, across))
    w_go(f, 0, across)
    near = sorted({k for k in (1, depth - 1) if 0 < k < depth})
    far = [k for k in range(1, depth) if k not in near]
    for k in near:
        w_go(f, k, column(k))

    cq_copy.wait()
    ck_copy.wait()
    first = (2 * chunks) // 3
    lax.fori_loop(0, first, multiply, 0)
    slot = depth
    for k in range(depth - 1, 0, -1):
        block = column(k)
        p_fs(block, 0, across).wait_recv()
        go(p_fs(block, slot, across))
        slot += 1
        go(p_tp(block, k))
    lax.fori_loop(first, chunks, multiply, 0)
    for k in range(depth):
        block = other(k)
        p_fs(block, 0, across).wait_recv()
        go(p_tp(block, depth + k))
    for k in range(depth):
        if k > 0:
            remote(pall.at[column(k), 1 - half], pall.at[column(k), 1 - half], s_send.at[0], s_recv.at[column(k)], (f, sibling)).wait_recv()
        remote(pall.at[other(k), 1 - half], pall.at[other(k), 1 - half], s_send.at[0], s_recv.at[other(k)], (f, sibling)).wait_recv()

    whole_p = pall[...].reshape(n * rows, pall.shape[-1])
    projected = jnp.dot(acc[...].astype(BF16), whole_p, preferred_element_type=F32).T
    for k in range(n):
        piece = projected[k * rr : (k + 1) * rr]
        rs_mine[k] = piece
        rs_send[k] = piece.astype(BF16)
    for k in range(1, n):
        to = lax.rem(f + k, n)
        go(remote(rs_send.at[to], rs_recv.at[f], rs_ssem.at[k], rs_rsem.at[f], (to, t)))
    for k in far:
        w_go(f, k, column(k))
    for k in near:
        block = column(depth - k)
        w_wait(block)
        w_go(block, depth + k, across)
    total = rs_mine[f]
    for k in range(1, n):
        src = lax.rem(f + n - k, n)
        remote(rs_recv.at[src], rs_recv.at[src], rs_ssem.at[0], rs_rsem.at[src], (f, sibling)).wait_recv()
        total = total + rs_recv[src].astype(F32)

    total_ref[...] = total
    (_, _, dir_q), (_, _, dir_k) = directions(total, qw, mq_ref, mk_ref, vq_ref, vk_ref)
    dall[f] = jnp.concatenate([dir_q, dir_k], axis=1).astype(BF16)
    lane = lax.broadcasted_iota(jnp.int32, (1, 128), 1)
    sums[me] = jnp.where(lane < 64, jnp.sum(dir_q * dir_q), jnp.sum(dir_k * dir_k))
    for k in range(1, n):
        to = lax.rem(f + k, n)
        go(remote(dall.at[f], dall.at[f], d_send.at[k], d_recv.at[f], (to, t)))
    for i in range(n):
        for j in range(tp):
            if i or j:
                to = (lax.rem(f + i, n), lax.rem(t + j, tp))
                go(remote(sums.at[me], sums.at[me], q_send.at[i * tp + j], q_recv.at[me], to))

    for k in far:
        block = column(depth - k)
        w_wait(block)
        w_go(block, depth + k, across)
    for k in range(1, n):
        src = lax.rem(f + n - k, n)
        remote(dall.at[src], dall.at[src], d_send.at[0], d_recv.at[src], (f, sibling)).wait_recv()
    for i in range(n):
        for j in range(tp):
            if i or j:
                src = lax.rem(f + i, n) * tp + lax.rem(t + j, tp)
                remote(sums.at[src], sums.at[src], q_send.at[0], q_recv.at[src], (f, sibling)).wait_recv()
    for k in range(depth):
        w_wait(other(k))
    for copy in sends:
        copy.wait_send()


def finish(
    n,
    tp,
    pall,
    wqall,
    wkall,
    dall,
    sums,
    total_ref,
    wq_ref,
    wk_ref,
    mq_ref,
    mk_ref,
    vq_ref,
    vk_ref,
    qnew_ref,
    knew_ref,
    qstep_ref,
    kstep_ref,
    qcopy_ref,
    kcopy_ref,
    qfirst_ref,
    kfirst_ref,
    qsecond_ref,
    ksecond_ref,
):
    f = lax.axis_index("fs")
    rr, qw = mq_ref.shape
    kw = mk_ref.shape[1]
    rows = wk_ref.shape[0]
    query, latent = directions(total_ref[...], qw, mq_ref, mk_ref, vq_ref, vk_ref)
    qfirst_ref[...], qsecond_ref[...] = query[:2]
    kfirst_ref[...], ksecond_ref[...] = latent[:2]
    row = jnp.sum(sums[...], axis=0)
    q_count = jnp.float32(n * rr * qw * tp)
    k_count = jnp.float32(n * rr * kw * tp)
    q_scale = 0.5 * jnp.sqrt(q_count) / jnp.sqrt(row[:, 0:1] + 1e-06)
    k_scale = 0.5 * jnp.sqrt(k_count) / jnp.sqrt(row[:, 64:65] + 1e-06)
    dirs = jnp.concatenate([dall[k].astype(F32) for k in range(n)], axis=0)
    left = dirs[:, :qw].T.astype(BF16)
    right = dirs[:, qw:].astype(BF16)

    def steps(factor):
        step_q = lax.dot_general(left, factor, (((1,), (1,)), ((), ())), preferred_element_type=F32)
        return step_q * q_scale, jnp.dot(factor, right, preferred_element_type=F32) * k_scale

    def block(i):
        return pall[i].reshape(rows, pall.shape[-1])

    step_q, step_k = steps(block(f))
    qstep_ref[...] = step_q
    kstep_ref[...] = step_k
    qnew_ref[...] = wq_ref[...] - step_q
    knew_ref[...] = wk_ref[...] - step_k
    for i in range(n):
        step_q, step_k = steps(block(i))
        at = slice(i * rows, (i + 1) * rows)
        qcopy_ref[:, at] = (wqall[i].astype(F32) - step_q).astype(BF16)
        kcopy_ref[at, :] = (wkall[i].astype(F32) - step_k).astype(BF16)


def solution(mesh):
    n, tp = mesh.shape["fs"], mesh.shape["tp"]

    def body(x, cq, ck, factor, wq, wk, mq, mk, vq, vk):
        tokens, width = x.shape
        rows, rank = factor.shape
        qw, kw = wq.shape[1], wk.shape[1]
        lat = qw + kw
        rr = mq.shape[0]
        chunk = 512
        while tokens % chunk:
            chunk //= 2
        chunks = tokens // chunk
        vmem = pl.BlockSpec(memory_space=pltpu.VMEM)
        anys = pl.BlockSpec(memory_space=pl.ANY)
        dma = pltpu.SemaphoreType.DMA
        sds = jax.ShapeDtypeStruct
        small = (wq.T, wk, mq, mk, vq, vk)
        params = pltpu.CompilerParams
        arrays = pl.pallas_call(
            functools.partial(exchange, n, tp, chunks),
            out_shape=(
                sds((n, 2, rows // 2, rank), BF16),
                sds((n, qw, rows), BF16),
                sds((n, rows, kw), BF16),
                sds((n, rr, lat), BF16),
                sds((n * tp, 1, 128), F32),
                sds((rr, lat), F32),
            ),
            in_specs=[anys] * 4 + [vmem] * 6,
            out_specs=(vmem,) * 6,
            scratch_shapes=[
                pltpu.VMEM((chunks, chunk, width), BF16),
                pltpu.VMEM((qw, tokens), BF16),
                pltpu.VMEM((chunks, chunk, kw), BF16),
                pltpu.VMEM((lat, width), F32),
                pltpu.VMEM((n, rr, lat), F32),
                pltpu.VMEM((n, rr, lat), BF16),
                pltpu.VMEM((n, rr, lat), BF16),
                dma((chunks,)),
                dma((2,)),
                dma(()),
            ]
            + [dma((n,))] * 12
            + [dma((n * tp,))] * 2,
            compiler_params=params(
                collective_id=0, has_side_effects=True, vmem_limit_bytes=50 * 1024 * 1024
            ),
        )(
            x.reshape(chunks, chunk, width),
            cq.T,
            ck.reshape(chunks, chunk, kw),
            factor.reshape(2, rows // 2, rank),
            *small,
        )
        out = pl.pallas_call(
            functools.partial(finish, n, tp),
            out_shape=(
                sds((qw, rows), F32),
                sds((rows, kw), F32),
                sds((qw, rows), F32),
                sds((rows, kw), F32),
                sds((qw, n * rows), BF16),
                sds((n * rows, kw), BF16),
                sds((rr, qw), F32),
                sds((rr, kw), F32),
                sds((rr, qw), F32),
                sds((rr, kw), F32),
            ),
            in_specs=[vmem] * 12,
            out_specs=(vmem,) * 10,
            compiler_params=params(vmem_limit_bytes=40 * 1024 * 1024),
        )(*arrays, *small)
        return (out[0].T, out[1], out[2].T, out[3], out[4].T) + tuple(out[5:])

    return jax.shard_map(
        body,
        mesh=mesh,
        in_specs=(P("fs", None), P("fs", "tp"), P("fs", "tp"), P("fs", None)) + (P("fs", "tp"),) * 6,
        out_specs=(P("fs", "tp"),) * 4 + (P(None, "tp"),) * 2 + (P("fs", "tp"),) * 4,
        check_vma=False,
    )
```
